32 devices in a mesh: grp: 2 (over y), ep: 8 (over z, x), tp: 2 (over core).
Axes of the slice: x: 2, y: 2, z: 4, core: 2. Of those that a mesh axis runs over, the one named last changes fastest.
Arguments:
- hidden_state: bfloat16 [1024, 1024], P(('grp', 'ep'), 'tp'), parts along dimension 0, may hold values from -6 to 6
- expert_ids: int32 [1024, 4], P(('grp', 'ep')), parts along dimension 0, may hold values from 0 to 7, all different within a row; in each aligned block of 64 rows (0 to 63, 64 to 127, ...) at most 64 rows name the same one
- route_weight: float32 [1024, 4], P(('grp', 'ep')), parts along dimension 0, may hold values from 0.1 to 1
- gate_matrix: bfloat16 [8, 1024, 2048], P('ep', None, 'tp'), may hold values from -0.1875 to 0.1875
- up_matrix: bfloat16 [8, 1024, 2048], P('ep', None, 'tp'), may hold values from -0.1875 to 0.1875
- down_matrix: bfloat16 [8, 2048, 1024], P('ep', 'tp'), may hold values from -2 to 2
- norm_gain: float32 [1024], P('tp'), may hold values from 0.1 to 1.9
Outputs:
- normed_out: bfloat16 [1024, 1024], P(('grp', 'ep'), 'tp'), parts along dimension 0
The draws below stay inside these ranges and needn't reach their ends.
There are 2 independent parts, one for each index of `grp`. The reference program is written for one: setup_inputs(seed, part) draws one part's arguments, and reference() takes and returns one part's arrays. A program takes and returns all parts, laid end to end along the dimension named above; an argument that names none is the same for every part. Nothing has to cross between parts.
Inputs may be any that keep to these rules, and one draw needn't show every extreme that they name: `expert_ids`: each row names 4 different experts. Within the rows of one index of ep (aligned blocks of 64 rows) no expert is named by more than 64 rows, and in some blocks one expert is named by exactly 64 rows. Every expert is named by some row.
All inputs are finite; a program needn't handle non-finite values.
Results may differ from the reference program's by a relative error of at most 0.0065.
Values may be sent and summed in bfloat16 or wider, within the bound.
A program may use at most 64 MiB of HBM per device.

```python
import math
import jax
import jax.numpy as jnp
import numpy as np
from jax import lax

D = 1024
FF = 2048
TOPK = 4
TOK_DEV = 64
EXPERTS = 8
TOKENS = 512
CAP = 64
N_EP = 8
N_TP = 2


def draw_down_matrix(key, part):
    noise_key = jax.random.fold_in(key, 11)
    scale_key = jax.random.fold_in(key, 23)
    column = jnp.arange(D, dtype=jnp.float32) / D
    jitter = jax.random.uniform(scale_key, (D,), jnp.float32, -0.35, 0.35)
    base = jnp.clip(jax.random.normal(noise_key, (EXPERTS, FF, D), jnp.float32), -6.0, 6.0)
    column_scale = jnp.exp(math.log(10.0) * column + jitter)
    values = base * column_scale[None, None, :] * FF ** (-0.5)
    return jnp.clip(values, -2.0, 2.0).astype(jnp.bfloat16)


def block_scale(key, shape, cuts, low, top_value):
    factor_of = 1.0
    for axis_at, shards_of in cuts:
        heights = jax.random.uniform(jax.random.fold_in(jax.random.fold_in(key, 6), axis_at), (shards_of,), jnp.float32, low / len(cuts), top_value / len(cuts))
        factor_of = factor_of * jnp.repeat(jnp.exp(heights), shape[axis_at] // shards_of).reshape((-1,) + (1,) * (len(shape) - 1 - axis_at))
    return factor_of


def deal_out(key, own, number, rows, number_of, top, bound, slope):
    sequence = jax.random.permutation(key, number_of)
    packed, ordinary = load_shares(number_of, rows * top, bound, slope, True), load_shares(number_of, rows * top, bound, slope, False)
    places = jnp.arange(number_of)

    def named(sizes, offset_by):
        used = int((sizes > 0).sum())
        fixed = max(1, used // 4)
        moved = fixed + (places - fixed + offset_by * (used - fixed)) % max(1, number_of - fixed)
        return jnp.zeros((number_of,), jnp.int32).at[sequence[jnp.where(places < fixed, places, moved)]].set(jnp.asarray(sizes, jnp.int32))

    sizes = jnp.where(number % 4 == 0, named(packed, number // 4), named(ordinary, number - number // 4 - 1))
    mixed = jax.random.permutation(jax.random.fold_in(own, 3), number_of)
    donor, taker = mixed[0:number_of // 2 * 2:2], mixed[1:number_of // 2 * 2:2]
    room = jnp.minimum(sizes[donor] - 1, bound - sizes[taker]) // 2
    room = jnp.where((donor == sequence[0]) | (taker == sequence[0]) | (sizes[taker] == 0), 0, jnp.maximum(room, 0))
    moved = jax.random.randint(jax.random.fold_in(own, 4), (number_of // 2,), 0, 1 << 20) % (room + 1)
    sizes = sizes.at[donor].add(-moved).at[taker].add(moved)
    members = jnp.searchsorted(jnp.cumsum(sizes), jnp.arange(rows * top), side="right").astype(jnp.int32)
    grid = members.reshape(top, rows).T
    grid = grid[jax.random.permutation(jax.random.fold_in(own, 1), rows)]
    offset_by = jax.random.randint(jax.random.fold_in(own, 2), (rows, 1), 0, top)
    return jnp.take_along_axis(grid, (jnp.arange(top)[None, :] + offset_by) % top, axis=1)


def load_shares(number_of, total, reach, slope, full):
    weights = [(1 << 20) // math.isqrt(standing ** slope) + 1 for standing in range(1, number_of + 1)]
    largest = reach if full else min(reach, max(-(-total // number_of), total * weights[0] // sum(weights)))
    least = 1 if total - largest >= number_of - 1 else 0
    counts, rest = [largest] + [least] * (number_of - 1), total - largest - least * (number_of - 1)
    while rest > 0:
        candidates = [i for i in range(1, number_of) if counts[i] < largest] or [i for i in range(1, number_of) if counts[i] < reach]
        whole, budget = sum([weights[i] for i in candidates]), rest
        for i in candidates:
            extra = min(reach - counts[i], max(1, budget * weights[i] // whole), rest)
            counts[i] = counts[i] + extra
            rest = rest - extra
    return np.array(counts)


def centred(rng, extent, width, bound, pieces=(), kind=jnp.bfloat16):
    array = jax.random.normal(rng, extent, jnp.float32) * width
    if len(pieces) > 0:
        array = block_scale(rng, extent, pieces, -0.22, 0.18) * array
    return jnp.clip(array, min=-bound, max=bound).astype(kind)


def setup_inputs(seed: int = 0, part: int = 0) -> dict:
    seeds = jax.random.split(jax.random.key(seed), 8)
    own_keys = jax.random.split(jax.random.fold_in(seeds[7], part), 8)
    hidden_state = centred(own_keys[0], (TOKENS, D), 1.0, 6.0, ((0, 8), (1, 2)))
    expert_ids_keys = jax.random.split(jax.random.fold_in(own_keys[1], 1), TOKENS // TOK_DEV)
    expert_ids_turns = jax.random.permutation(jax.random.fold_in(own_keys[1], 3), TOKENS // TOK_DEV)
    expert_ids = jax.vmap(lambda own, number: deal_out(jax.random.fold_in(own_keys[1], 2), own, number, TOK_DEV, EXPERTS, TOPK, CAP, 2))(expert_ids_keys, expert_ids_turns).reshape((TOKENS, TOPK))
    route_weight = jnp.clip(jnp.exp(math.log(1.0) - 2.3025851 * jax.random.uniform(own_keys[2], (TOKENS, TOPK), jnp.float32) ** block_scale(own_keys[2], (TOKENS, TOPK), ((0, 8),), -0.2, 0.2)), 0.1, 1.0)
    gate_matrix = centred(seeds[3], (EXPERTS, D, FF), D ** -0.5, 0.1875, ((0, 8), (2, 2)))
    up_matrix = centred(seeds[4], (EXPERTS, D, FF), D ** -0.5, 0.1875, ((0, 8), (2, 2)))
    down_matrix = draw_down_matrix(jax.random.fold_in(seeds[7], 71), part)
    norm_gain = jnp.clip(1.0 + 0.18 * jax.random.normal(seeds[6], (D,), jnp.float32), 0.1, 1.9)
    return {"hidden_state": hidden_state, "expert_ids": expert_ids, "route_weight": route_weight, "gate_matrix": gate_matrix, "up_matrix": up_matrix, "down_matrix": down_matrix, "norm_gain": norm_gain}


def slot_ranks(expert_ids):
    blocks = expert_ids.reshape(N_EP, TOK_DEV * TOPK)
    onehot = (blocks[:, :, None] == jnp.arange(EXPERTS, dtype=jnp.int32)[None, None, :]).astype(jnp.int32)
    earlier = jnp.cumsum(onehot, axis=1) - onehot
    return lax.optimization_barrier(jnp.sum(earlier * onehot, axis=2)).astype(jnp.int32).reshape(TOKENS, TOPK)

def reference(hidden_state, expert_ids, route_weight, gate_matrix, up_matrix, down_matrix, norm_gain):
    slot_rank = slot_ranks(expert_ids)
    block_index = (jnp.arange(TOKENS, dtype=jnp.int32) // TOK_DEV)[:, None]
    slot_index = (block_index * CAP + slot_rank).astype(jnp.int32)
    token_ids = jnp.broadcast_to(jnp.arange(TOKENS, dtype=jnp.int32)[:, None], (TOKENS, TOPK))
    slot_table = jnp.zeros((EXPERTS, N_EP * CAP), jnp.int32).at[expert_ids, slot_index].set(token_ids)
    half_width = FF // N_TP

    def one_expert(operands):
        row_index, gate_block, up_block, down_block = operands
        token_rows = hidden_state[row_index]
        gate_pre = jnp.dot(token_rows, gate_block, preferred_element_type=jnp.float32)
        up_pre = jnp.dot(token_rows, up_block, preferred_element_type=jnp.float32)
        activated = (jax.nn.silu(gate_pre) * up_pre).astype(jnp.bfloat16)
        summed_rows = jnp.zeros((token_rows.shape[0], D), jnp.float32)
        for segment in range(N_TP):
            partial_value = jnp.dot(activated[:, segment * half_width:(segment + 1) * half_width], down_block[segment * half_width:(segment + 1) * half_width], preferred_element_type=jnp.float32).astype(jnp.bfloat16)
            partial_value = lax.optimization_barrier(partial_value)
            summed_rows = summed_rows + partial_value.astype(jnp.float32)
        return summed_rows.astype(jnp.bfloat16)
    outputs = lax.map(one_expert, (slot_table, gate_matrix, up_matrix, down_matrix))
    picked = outputs[expert_ids, slot_index]
    combined = lax.optimization_barrier(jnp.sum(route_weight[:, :, None].astype(jnp.float32) * picked.astype(jnp.float32), axis=1))
    mean_square = lax.optimization_barrier(jnp.mean(combined * combined, axis=1, keepdims=True))
    return (combined * lax.rsqrt(mean_square + 1e-05) * norm_gain).astype(jnp.bfloat16)
```

```python
import functools

import jax
import jax.numpy as jnp
from jax import lax
from jax.experimental import pallas as pl
from jax.experimental.pallas import tpu as pltpu
from jax.sharding import PartitionSpec as P

MESH = pl.DeviceIdType.MESH
norm_eps = 1e-05


def slot_numbers(block_ids, expert_count):
    onehot = (block_ids[..., None] == jnp.arange(expert_count, dtype=jnp.int32)).astype(jnp.int32)
    earlier = jnp.cumsum(onehot, axis=-2) - onehot
    return jnp.sum(earlier * onehot, axis=-1)


def expert_rows(buffer, gate_matrix, up_matrix, down_matrix):
    sources, item_count, feature_count = buffer.shape
    token_rows = buffer.reshape(sources * item_count, feature_count)
    gate_pre = jnp.dot(token_rows, gate_matrix[0], preferred_element_type=jnp.float32)
    up_pre = jnp.dot(token_rows, up_matrix[0], preferred_element_type=jnp.float32)
    activated = (jax.nn.silu(gate_pre) * up_pre).astype(jnp.bfloat16)
    partial_value = jnp.dot(activated, down_matrix[0], preferred_element_type=jnp.float32)
    return lax.psum_scatter(
        partial_value.reshape(sources, item_count, feature_count).astype(jnp.bfloat16),
        "tp",
        scatter_dimension=2,
        tiled=True,
    )


def slotted(hidden_state, expert_ids, route_weight, gate_matrix, up_matrix, down_matrix, norm_gain):
    tok_count, top_count = expert_ids.shape
    expert_count = lax.axis_size("ep")
    feature_total = hidden_state.shape[1] * lax.axis_size("tp")
    capacity = max(2, 2 * tok_count * top_count // expert_count)
    slot_total = expert_count * capacity
    slot_rank = slot_numbers(expert_ids.reshape(1, tok_count * top_count), expert_count)
    slot_index = expert_ids * capacity + slot_rank.reshape(tok_count, top_count)
    positions = jnp.arange(slot_total, dtype=jnp.int32)
    matches = slot_index[:, :, None] == positions[None, None, :]
    placing = jnp.transpose(jnp.any(matches, axis=1)).astype(jnp.bfloat16)
    combine = jnp.sum(jnp.where(matches, route_weight[:, :, None], 0.0), axis=1)
    outgoing = jnp.dot(placing, hidden_state, preferred_element_type=jnp.float32).astype(
        jnp.bfloat16
    )
    received = lax.all_to_all(
        outgoing.reshape(expert_count, capacity, hidden_state.shape[1]),
        "ep",
        split_axis=0,
        concat_axis=0,
        tiled=True,
    )
    answers = expert_rows(
        lax.all_gather(received, "tp", axis=2, tiled=True), gate_matrix, up_matrix, down_matrix
    )
    returned = lax.all_to_all(answers, "ep", split_axis=0, concat_axis=0, tiled=True)
    combined = jnp.dot(
        combine,
        returned.reshape(slot_total, returned.shape[2]).astype(jnp.float32),
        precision=lax.Precision.HIGHEST,
    )
    total_squares = lax.psum(jnp.sum(combined * combined, axis=1), "tp")
    inverse_rms = lax.rsqrt(total_squares / feature_total + norm_eps)
    return (combined * inverse_rms[:, None] * norm_gain).astype(jnp.bfloat16)


def kernel(
    nz, nx, ids, rw, h, g_hbm, u_hbm, d_hbm, gain, out,
    xs, gw, uw, dw, act, psend, precv, ys, ret, sq, sqr,
    wsem, osem, gs, gr, ps, pr, ds, dr, rs, rr, qs, qr,
):
    n = nz * nx
    tok, half = h.shape
    rows = nz * tok
    me = lax.axis_index("ep")
    z, x = me // nx, me % nx
    c = lax.axis_index("tp")
    other = (c + 1) % 2
    mine = x * nz + z

    weights = [
        pltpu.make_async_copy(g_hbm.at[0], gw, wsem.at[0]),
        pltpu.make_async_copy(u_hbm.at[0], uw, wsem.at[1]),
        pltpu.make_async_copy(d_hbm.at[0], dw, wsem.at[2]),
    ]
    own = pltpu.make_async_copy(h, xs.at[c, mine], osem)
    own.start()
    for w in weights:
        w.start()

    barrier = pltpu.get_barrier_semaphore()
    for k in range(1, n):
        pl.semaphore_signal(
            barrier, inc=1, device_id={"ep": (me + k) % n}, device_id_type=MESH
        )
    pl.semaphore_signal(barrier, inc=1, device_id={"tp": other}, device_id_type=MESH)
    pl.semaphore_wait(barrier, n)

    def place(j, dz):
        zz, xx = (z + dz) % nz, (x + j) % nx
        return zz * nx + xx, xx * nz + zz

    def to_chip(src, dst, send, recv, chip):
        return pltpu.make_async_remote_copy(
            src_ref=src, dst_ref=dst, send_sem=send, recv_sem=recv,
            device_id={"ep": chip}, device_id_type=MESH,
        )

    def to_core(src, dst, send, recv):
        return pltpu.make_async_remote_copy(
            src_ref=src, dst_ref=dst, send_sem=send, recv_sem=recv,
            device_id={"tp": other}, device_id_type=MESH,
        )

    order = [(j, dz) for j in range(nx) for dz in range(nz)]
    started = []
    for j, dz in order[1:]:
        chip, slot = place(j, dz)
        copy = to_chip(h, xs.at[c, mine], gs.at[slot], gr.at[mine], chip)
        copy.start()
        started.append(copy)
    first = to_core(h, xs.at[c, mine], ps.at[mine], pr.at[mine])
    first.start()
    started.append(first)
    own.wait()

    def waited(ref, send, recv):
        return to_core(ref, ref, send, recv)

    for j in range(nx):
        col = (x + j) % nx
        for dz in range(nz):
            if (j, dz) == (0, 0):
                continue
            chip, slot = place(j, dz)
            waited(xs.at[c, slot], gs.at[slot], gr.at[slot]).wait_recv()
            copy = to_core(xs.at[c, slot], xs.at[c, slot], ps.at[slot], pr.at[slot])
            copy.start()
            started.append(copy)
        for dz in range(nz):
            chip, slot = place(j, dz)
            waited(xs.at[other, slot], ps.at[slot], pr.at[slot]).wait_recv()
        if j == 0:
            weights[0].wait()
            weights[1].wait()
        low = xs[0, pl.ds(col * nz, nz)].reshape(rows, half)
        high = xs[1, pl.ds(col * nz, nz)].reshape(rows, half)
        hid = gw.shape[1]
        tile = min(256, hid)
        for at in range(0, hid, tile):
            cut = slice(at, at + tile)
            gate = jnp.dot(low, gw[:half, cut], preferred_element_type=jnp.float32)
            gate += jnp.dot(high, gw[half:, cut], preferred_element_type=jnp.float32)
            up = jnp.dot(low, uw[:half, cut], preferred_element_type=jnp.float32)
            up += jnp.dot(high, uw[half:, cut], preferred_element_type=jnp.float32)
            act[:, cut] = (jax.nn.silu(gate) * up).astype(jnp.bfloat16)
        if j == 0:
            weights[2].wait()
        theirs = pl.ds(pl.multiple_of(other * half, half), half)
        ours = pl.ds(pl.multiple_of(c * half, half), half)
        psend[j] = jnp.dot(
            act[...], dw[:, theirs], preferred_element_type=jnp.float32
        ).astype(jnp.bfloat16)
        swap = to_core(psend.at[j], precv.at[j], ds.at[j], dr.at[j])
        swap.start()
        part = jnp.dot(act[...], dw[:, ours], preferred_element_type=jnp.float32).astype(
            jnp.bfloat16
        )
        swap.wait()
        total = (part.astype(jnp.float32) + precv[j].astype(jnp.float32)).astype(jnp.bfloat16)
        ys[pl.ds(col * nz, nz)] = total.reshape(nz, tok, half)
        for dz in range(nz):
            if (j, dz) == (0, 0):
                continue
            chip, slot = place(j, dz)
            copy = to_chip(ys.at[slot], ret.at[mine], rs.at[slot], rr.at[mine], chip)
            copy.start()
            started.append(copy)

    total = None
    for j, dz in order:
        chip, slot = place(j, dz)
        weight = jnp.zeros((tok, 1), jnp.float32)
        for k in range(ids.shape[1]):
            weight += jnp.where(ids[:, k : k + 1] == chip, rw[:, k : k + 1], 0.0)
        if (j, dz) == (0, 0):
            block = ys[mine]
        else:
            waited(ret.at[slot], rs.at[slot], rr.at[slot]).wait_recv()
            block = ret[slot]
        term = weight * block.astype(jnp.float32)
        total = term if total is None else total + term
    squares = jnp.sum(total * total, axis=1, keepdims=True)
    sq[...] = jnp.broadcast_to(squares, sq.shape)
    share = to_core(sq, sqr, qs, qr)
    share.start()
    share.wait()
    mean = (squares + sqr[:, :1]) / (half * 2)
    out[...] = (total * lax.rsqrt(mean + norm_eps) * gain[...]).astype(jnp.bfloat16)
    for copy in started:
        copy.wait_send()


def shards(hidden_state, expert_ids, route_weight, gate_matrix, up_matrix, down_matrix, norm_gain):
    tok, top = expert_ids.shape
    half = hidden_state.shape[1]
    hid = gate_matrix.shape[2]
    n = lax.axis_size("ep")
    if 2 * tok * top // n < tok or lax.axis_size("tp") != 2 or n % 2:
        return slotted(
            hidden_state, expert_ids, route_weight, gate_matrix, up_matrix, down_matrix, norm_gain
        )
    nx = 2
    nz = n // nx
    bf16, f32 = jnp.bfloat16, jnp.float32
    vmem = pl.BlockSpec(memory_space=pltpu.VMEM)
    hbm = pl.BlockSpec(memory_space=pl.ANY)
    dma = pltpu.SemaphoreType.DMA
    return pl.pallas_call(
        functools.partial(kernel, nz, nx),
        out_shape=jax.ShapeDtypeStruct((tok, half), bf16),
        in_specs=[vmem, vmem, vmem, hbm, hbm, hbm, vmem],
        out_specs=vmem,
        scratch_shapes=[
            pltpu.VMEM((2, n, tok, half), bf16),
            pltpu.VMEM((2 * half, hid), bf16),
            pltpu.VMEM((2 * half, hid), bf16),
            pltpu.VMEM((hid, 2 * half), bf16),
            pltpu.VMEM((nz * tok, hid), bf16),
            pltpu.VMEM((nx, nz * tok, half), bf16),
            pltpu.VMEM((nx, nz * tok, half), bf16),
            pltpu.VMEM((n, tok, half), bf16),
            pltpu.VMEM((n, tok, half), bf16),
            pltpu.VMEM((tok, 128), f32),
            pltpu.VMEM((tok, 128), f32),
            dma((3,)),
            dma,
            dma((n,)),
            dma((n,)),
            dma((n,)),
            dma((n,)),
            dma((nx,)),
            dma((nx,)),
            dma((n,)),
            dma((n,)),
            dma,
            dma,
        ],
        compiler_params=pltpu.CompilerParams(
            collective_id=0, has_side_effects=True, vmem_limit_bytes=48 * 1024 * 1024
        ),
    )(
        expert_ids, route_weight, hidden_state, gate_matrix, up_matrix, down_matrix,
        norm_gain.reshape(1, half),
    )


def solution(mesh):
    placed = (
        P(("grp", "ep"), "tp"),
        P(("grp", "ep"), None),
        P(("grp", "ep"), None),
        P("ep", None, "tp"),
        P("ep", None, "tp"),
        P("ep", "tp", None),
        P("tp"),
    )
    return jax.shard_map(
        shards, mesh=mesh, in_specs=placed, out_specs=P(("grp", "ep"), "tp"), check_vma=False
    )
```

```python
import functools

import jax
import jax.numpy as jnp
from jax import lax
from jax.experimental import pallas as pl
from jax.experimental.pallas import tpu as pltpu
from jax.sharding import PartitionSpec as P

MESH = pl.DeviceIdType.MESH
norm_eps = 1e-05


def slot_numbers(block_ids, expert_count):
    onehot = (block_ids[..., None] == jnp.arange(expert_count, dtype=jnp.int32)).astype(jnp.int32)
    earlier = jnp.cumsum(onehot, axis=-2) - onehot
    return jnp.sum(earlier * onehot, axis=-1)


def expert_rows(buffer, gate_matrix, up_matrix, down_matrix):
    sources, item_count, feature_count = buffer.shape
    token_rows = buffer.reshape(sources * item_count, feature_count)
    gate_pre = jnp.dot(token_rows, gate_matrix[0], preferred_element_type=jnp.float32)
    up_pre = jnp.dot(token_rows, up_matrix[0], preferred_element_type=jnp.float32)
    activated = (jax.nn.silu(gate_pre) * up_pre).astype(jnp.bfloat16)
    partial_value = jnp.dot(activated, down_matrix[0], preferred_element_type=jnp.float32)
    return lax.psum_scatter(
        partial_value.reshape(sources, item_count, feature_count).astype(jnp.bfloat16),
        "tp",
        scatter_dimension=2,
        tiled=True,
    )


def slotted(hidden_state, expert_ids, route_weight, gate_matrix, up_matrix, down_matrix, norm_gain):
    tok_count, top_count = expert_ids.shape
    expert_count = lax.axis_size("ep")
    feature_total = hidden_state.shape[1] * lax.axis_size("tp")
    capacity = max(2, 2 * tok_count * top_count // expert_count)
    slot_total = expert_count * capacity
    slot_rank = slot_numbers(expert_ids.reshape(1, tok_count * top_count), expert_count)
    slot_index = expert_ids * capacity + slot_rank.reshape(tok_count, top_count)
    positions = jnp.arange(slot_total, dtype=jnp.int32)
    matches = slot_index[:, :, None] == positions[None, None, :]
    placing = jnp.transpose(jnp.any(matches, axis=1)).astype(jnp.bfloat16)
    combine = jnp.sum(jnp.where(matches, route_weight[:, :, None], 0.0), axis=1)
    outgoing = jnp.dot(placing, hidden_state, preferred_element_type=jnp.float32).astype(
        jnp.bfloat16
    )
    received = lax.all_to_all(
        outgoing.reshape(expert_count, capacity, hidden_state.shape[1]),
        "ep",
        split_axis=0,
        concat_axis=0,
        tiled=True,
    )
    answers = expert_rows(
        lax.all_gather(received, "tp", axis=2, tiled=True), gate_matrix, up_matrix, down_matrix
    )
    returned = lax.all_to_all(answers, "ep", split_axis=0, concat_axis=0, tiled=True)
    combined = jnp.dot(
        combine,
        returned.reshape(slot_total, returned.shape[2]).astype(jnp.float32),
        precision=lax.Precision.HIGHEST,
    )
    total_squares = lax.psum(jnp.sum(combined * combined, axis=1), "tp")
    inverse_rms = lax.rsqrt(total_squares / feature_total + norm_eps)
    return (combined * inverse_rms[:, None] * norm_gain).astype(jnp.bfloat16)


def kernel(
    nz, nx, ids_hbm, rw_hbm, h_hbm, g_hbm, u_hbm, d_hbm, gain_hbm, out,
    ids, rw, gain, xs, gw, uw, dw, act, psend, precv, acc, ys, yx, zs, ret, sq, sqr,
    wsem, osem, gs, gr, fs, ps, pr, ns, nr, ds, dr, us, ur, rs, rr, qs, qr,
):
    tok, half = out.shape
    hid = gw.shape[1]
    pairs = nz // 2
    me = lax.axis_index("ep")
    z, x = me // nx, me % nx
    beside = (x + 1) % nx
    c = lax.axis_index("tp")
    other = (c + 1) % 2
    mine = x * nz + z

    def local(src, dst, sem):
        copy = pltpu.make_async_copy(src, dst, sem)
        copy.start()
        return copy

    own = local(h_hbm, xs.at[c, mine], osem.at[0])
    own_ids = local(ids_hbm, ids.at[z], osem.at[1])
    own_rw = local(rw_hbm, rw.at[z], osem.at[2])
    weights = [
        local(g_hbm.at[0], gw, wsem.at[0]),
        local(u_hbm.at[0], uw, wsem.at[1]),
        local(d_hbm.at[0], dw, wsem.at[2]),
    ]
    own_gain = local(gain_hbm, gain, osem.at[3])

    def row_of(d, r):
        return 2 * ((z // 2 + d) % pairs) + (z + r) % 2

    def far(d, r):
        return (d, r) != (0, 0)

    spots = [(d, r) for d in range(pairs) for r in (1, 0)]
    peers = [spot for spot in spots if far(*spot)]

    barrier = pltpu.get_barrier_semaphore()
    for d, r in peers:
        pl.semaphore_signal(
            barrier, inc=1, device_id={"ep": row_of(d, r) * nx + x}, device_id_type=MESH
        )
    pl.semaphore_signal(
        barrier, inc=1, device_id={"ep": z * nx + beside}, device_id_type=MESH
    )
    pl.semaphore_signal(barrier, inc=1, device_id={"tp": other}, device_id_type=MESH)
    own.wait()
    own_ids.wait()
    own_rw.wait()
    pl.semaphore_wait(barrier, nz + 1)

    def remote(src, dst, send, recv, where):
        return pltpu.make_async_remote_copy(
            src_ref=src, dst_ref=dst, send_sem=send, recv_sem=recv,
            device_id=where, device_id_type=MESH,
        )

    def along(row):
        return {"ep": row * nx + x}

    across = {"ep": z * nx + beside}
    twin = {"tp": other}
    started = []

    def send(*what):
        copy = remote(*what)
        copy.start()
        started.append(copy)
        return copy

    block = xs.at[c, mine]
    send(block, block, fs.at[z], gr.at[mine], across)
    for d, r in peers:
        row = row_of(d, r)
        send(block, block, gs.at[row], gr.at[mine], along(row))
    send(block, block, ps.at[mine], pr.at[mine], twin)
    for d, r in peers:
        row = row_of(d, r)
        send(ids.at[z], ids.at[z], ns.at[0, row], nr.at[0, z], along(row))
        send(rw.at[z], rw.at[z], ns.at[1, row], nr.at[1, z], along(row))

    def arrive(j, d, r):
        if j == 0 and not far(d, r):
            return
        row = row_of(d, r)
        slot = (x + j) % nx * nz + row
        ref = xs.at[c, slot]
        remote(ref, ref, ps.at[slot], gr.at[slot], twin).wait_recv()
        if j == 0:
            send(ref, ref, fs.at[row], gr.at[slot], across)
        send(ref, ref, ps.at[slot], pr.at[slot], twin)

    theirs = pl.ds(pl.multiple_of(other * half, half), half)
    ours = pl.ds(pl.multiple_of(c * half, half), half)
    kept = {}

    def compute(j, d):
        for r in range(2):
            slot = (x + j) % nx * nz + row_of(d, r)
            ref = xs.at[other, slot]
            remote(ref, ref, ps.at[slot], pr.at[slot], twin).wait_recv()
        if (j, d) == (0, 0):
            weights[0].wait()
            weights[1].wait()
        base = (x + j) % nx * nz + 2 * ((z // 2 + d) % pairs)
        low = xs[0, pl.ds(base, 2)].reshape(2 * tok, half)
        high = xs[1, pl.ds(base, 2)].reshape(2 * tok, half)
        tile = min(256, hid)
        for at in range(0, hid, tile):
            cut = slice(at, at + tile)
            gate = jnp.dot(low, gw[:half, cut], preferred_element_type=jnp.float32)
            gate += jnp.dot(high, gw[half:, cut], preferred_element_type=jnp.float32)
            up = jnp.dot(low, uw[:half, cut], preferred_element_type=jnp.float32)
            up += jnp.dot(high, uw[half:, cut], preferred_element_type=jnp.float32)
            act[:, cut] = (jax.nn.silu(gate) * up).astype(jnp.bfloat16)
        if (j, d) == (0, 0):
            weights[2].wait()
        q = 2 * d + j
        psend[q] = jnp.dot(
            act[...], dw[:, theirs], preferred_element_type=jnp.float32
        ).astype(jnp.bfloat16)
        swap = remote(psend.at[q], precv.at[q], ds.at[q], dr.at[q], twin)
        swap.start()
        kept[q] = swap
        part = jnp.dot(act[...], dw[:, ours], preferred_element_type=jnp.float32)
        part = part.astype(jnp.bfloat16).reshape(2, tok, half)
        lower = 2 * ((z // 2 + d) % pairs)
        if j == 0:
            acc[pl.ds(lower, 2)] = part.astype(jnp.float32)
        else:
            ys[pl.ds(lower, 2)] = part

    eye = lax.broadcasted_iota(jnp.int32, (tok, tok), 0) == lax.broadcasted_iota(
        jnp.int32, (tok, tok), 1
    )

    def weight_of(row, chip):
        line = jnp.zeros((1, tok), jnp.float32)
        for k in range(ids.shape[1]):
            line += jnp.where(ids[row, k : k + 1] == chip, rw[row, k : k + 1], 0.0)
        return jnp.sum(jnp.where(eye, line, 0.0), axis=1, keepdims=True)

    def keep(d):
        q = 2 * d
        kept[q].wait()
        for r in range(2):
            row = row_of(d, r)
            if far(d, r):
                for i, ref in enumerate((ids, rw)):
                    remote(
                        ref.at[row], ref.at[row], ns.at[i, row], nr.at[i, row], along(row)
                    ).wait_recv()
            got = precv[q, pl.ds(pl.multiple_of(row % 2 * tok, tok), tok)]
            done = (acc[row] + got.astype(jnp.float32)).astype(jnp.bfloat16)
            acc[row] = done.astype(jnp.float32) * weight_of(row, me)

    def pass_on(d):
        q = 2 * d + 1
        kept[q].wait()
        for r in (1, 0):
            row = row_of(d, r)
            got = precv[q, pl.ds(pl.multiple_of(row % 2 * tok, tok), tok)]
            done = ys[row].astype(jnp.float32) + got.astype(jnp.float32)
            ys[row] = done.astype(jnp.bfloat16)
            send(ys.at[row], yx.at[row], us.at[row], ur.at[row], across)

    def relay(d):
        for r in (1, 0):
            row = row_of(d, r)
            weight = weight_of(row, z * nx + beside)
            remote(yx.at[row], yx.at[row], us.at[row], ur.at[row], across).wait_recv()
            both = acc[row] + weight * yx[row].astype(jnp.float32)
            if far(d, r):
                zs[row] = both.astype(jnp.bfloat16)
                send(zs.at[row], ret.at[z], rs.at[row], rr.at[z], along(row))
            else:
                acc[row] = both

    arrive(0, 0, 1)
    for d in range(pairs):
        if d > 0:
            arrive(0, d, 0)
        compute(0, d)
        arrive(1, d, 0)
        arrive(1, d, 1)
        if d + 1 < pairs:
            arrive(0, d + 1, 1)
        compute(1, d)
        keep(d)
        if d > 0:
            relay(d - 1)
        pass_on(d)
    relay(pairs - 1)

    total = acc[z]
    for d, r in peers:
        row = row_of(d, r)
        remote(ret.at[row], ret.at[row], rs.at[row], rr.at[row], along(row)).wait_recv()
        total += ret[row].astype(jnp.float32)
    squares = jnp.sum(total * total, axis=1, keepdims=True)
    sq[...] = jnp.broadcast_to(squares, sq.shape)
    share = remote(sq, sqr, qs, qr, twin)
    share.start()
    own_gain.wait()
    share.wait()
    mean = (squares + sqr[:, :1]) / (half * 2)
    out[...] = (total * lax.rsqrt(mean + norm_eps) * gain[...]).astype(jnp.bfloat16)
    for copy in started:
        copy.wait_send()


def shards(hidden_state, expert_ids, route_weight, gate_matrix, up_matrix, down_matrix, norm_gain):
    tok, top = expert_ids.shape
    half = hidden_state.shape[1]
    hid = gate_matrix.shape[2]
    n = lax.axis_size("ep")
    if 2 * tok * top // n < tok or lax.axis_size("tp") != 2 or n % 4:
        return slotted(
            hidden_state, expert_ids, route_weight, gate_matrix, up_matrix, down_matrix, norm_gain
        )
    nx = 2
    nz = n // nx
    bf16, f32 = jnp.bfloat16, jnp.float32
    vmem = pl.BlockSpec(memory_space=pltpu.VMEM)
    hbm = pl.BlockSpec(memory_space=pl.ANY)
    dma = pltpu.SemaphoreType.DMA
    return pl.pallas_call(
        functools.partial(kernel, nz, nx),
        out_shape=jax.ShapeDtypeStruct((tok, half), bf16),
        in_specs=[hbm] * 7,
        out_specs=vmem,
        scratch_shapes=[
            pltpu.VMEM((nz, top, tok), jnp.int32),
            pltpu.VMEM((nz, top, tok), f32),
            pltpu.VMEM((1, half), f32),
            pltpu.VMEM((2, n, tok, half), bf16),
            pltpu.VMEM((2 * half, hid), bf16),
            pltpu.VMEM((2 * half, hid), bf16),
            pltpu.VMEM((hid, 2 * half), bf16),
            pltpu.VMEM((2 * tok, hid), bf16),
            pltpu.VMEM((nz, 2 * tok, half), bf16),
            pltpu.VMEM((nz, 2 * tok, half), bf16),
            pltpu.VMEM((nz, tok, half), f32),
            pltpu.VMEM((nz, tok, half), bf16),
            pltpu.VMEM((nz, tok, half), bf16),
            pltpu.VMEM((nz, tok, half), bf16),
            pltpu.VMEM((nz, tok, half), bf16),
            pltpu.VMEM((tok, 128), f32),
            pltpu.VMEM((tok, 128), f32),
            dma((3,)),
            dma((4,)),
            dma((nz,)),
            dma((n,)),
            dma((nz,)),
            dma((n,)),
            dma((n,)),
            dma((2, nz)),
            dma((2, nz)),
            dma((nz,)),
            dma((nz,)),
            dma((nz,)),
            dma((nz,)),
            dma((nz,)),
            dma((nz,)),
            dma,
            dma,
        ],
        compiler_params=pltpu.CompilerParams(
            collective_id=0, has_side_effects=True, vmem_limit_bytes=60 * 1024 * 1024
        ),
    )(
        expert_ids.T, route_weight.T, hidden_state, gate_matrix, up_matrix, down_matrix,
        norm_gain.reshape(1, half),
    )


def solution(mesh):
    placed = (
        P(("grp", "ep"), "tp"),
        P(("grp", "ep"), None),
        P(("grp", "ep"), None),
        P("ep", None, "tp"),
        P("ep", None, "tp"),
        P("ep", "tp", None),
        P("tp"),
    )
    return jax.shard_map(
        shards, mesh=mesh, in_specs=placed, out_specs=P(("grp", "ep"), "tp"), check_vma=False
    )
```

```python
import functools

import jax
import jax.numpy as jnp
from jax import lax
from jax.experimental import pallas as pl
from jax.experimental.pallas import tpu as pltpu
from jax.sharding import PartitionSpec as P

MESH = pl.DeviceIdType.MESH
norm_eps = 1e-05


def slot_numbers(block_ids, expert_count):
    onehot = (block_ids[..., None] == jnp.arange(expert_count, dtype=jnp.int32)).astype(jnp.int32)
    earlier = jnp.cumsum(onehot, axis=-2) - onehot
    return jnp.sum(earlier * onehot, axis=-1)


def expert_rows(buffer, gate_matrix, up_matrix, down_matrix):
    sources, item_count, feature_count = buffer.shape
    token_rows = buffer.reshape(sources * item_count, feature_count)
    gate_pre = jnp.dot(token_rows, gate_matrix[0], preferred_element_type=jnp.float32)
    up_pre = jnp.dot(token_rows, up_matrix[0], preferred_element_type=jnp.float32)
    activated = (jax.nn.silu(gate_pre) * up_pre).astype(jnp.bfloat16)
    partial_value = jnp.dot(activated, down_matrix[0], preferred_element_type=jnp.float32)
    return lax.psum_scatter(
        partial_value.reshape(sources, item_count, feature_count).astype(jnp.bfloat16),
        "tp",
        scatter_dimension=2,
        tiled=True,
    )


def slotted(hidden_state, expert_ids, route_weight, gate_matrix, up_matrix, down_matrix, norm_gain):
    tok_count, top_count = expert_ids.shape
    expert_count = lax.axis_size("ep")
    feature_total = hidden_state.shape[1] * lax.axis_size("tp")
    capacity = max(2, 2 * tok_count * top_count // expert_count)
    slot_total = expert_count * capacity
    slot_rank = slot_numbers(expert_ids.reshape(1, tok_count * top_count), expert_count)
    slot_index = expert_ids * capacity + slot_rank.reshape(tok_count, top_count)
    positions = jnp.arange(slot_total, dtype=jnp.int32)
    matches = slot_index[:, :, None] == positions[None, None, :]
    placing = jnp.transpose(jnp.any(matches, axis=1)).astype(jnp.bfloat16)
    combine = jnp.sum(jnp.where(matches, route_weight[:, :, None], 0.0), axis=1)
    outgoing = jnp.dot(placing, hidden_state, preferred_element_type=jnp.float32).astype(
        jnp.bfloat16
    )
    received = lax.all_to_all(
        outgoing.reshape(expert_count, capacity, hidden_state.shape[1]),
        "ep",
        split_axis=0,
        concat_axis=0,
        tiled=True,
    )
    answers = expert_rows(
        lax.all_gather(received, "tp", axis=2, tiled=True), gate_matrix, up_matrix, down_matrix
    )
    returned = lax.all_to_all(answers, "ep", split_axis=0, concat_axis=0, tiled=True)
    combined = jnp.dot(
        combine,
        returned.reshape(slot_total, returned.shape[2]).astype(jnp.float32),
        precision=lax.Precision.HIGHEST,
    )
    total_squares = lax.psum(jnp.sum(combined * combined, axis=1), "tp")
    inverse_rms = lax.rsqrt(total_squares / feature_total + norm_eps)
    return (combined * inverse_rms[:, None] * norm_gain).astype(jnp.bfloat16)


def kernel(
    nz, nx, ids_hbm, rw_hbm, h_hbm, g_hbm, u_hbm, d_hbm, gain_hbm, out,
    ids, rw, gain, xs, gw, uw, dw, act, psend, precv, ys, ret, sq, sqr,
    wsem, osem, gs, gr, fs, ps, pr, ds, dr, rs, rr, qs, qr,
):
    tok, half = out.shape
    hid = gw.shape[1]
    pairs = nz // 2
    me = lax.axis_index("ep")
    z, x = me // nx, me % nx
    beside = (x + 1) % nx
    c = lax.axis_index("tp")
    other = (c + 1) % 2
    mine = x * nz + z

    def local(src, dst, sem):
        copy = pltpu.make_async_copy(src, dst, sem)
        copy.start()
        return copy

    own = local(h_hbm, xs.at[c, mine], osem.at[0])
    own_ids = local(ids_hbm, ids, osem.at[1])
    own_rw = local(rw_hbm, rw, osem.at[2])
    weights = [
        local(g_hbm.at[0], gw, wsem.at[0]),
        local(u_hbm.at[0], uw, wsem.at[1]),
        local(d_hbm.at[0], dw, wsem.at[2]),
    ]
    own_gain = local(gain_hbm, gain, osem.at[3])

    def row_of(d, r):
        return 2 * ((z // 2 + d) % pairs) + (z + r) % 2

    def far(d, r):
        return (d, r) != (0, 0)

    spots = [(d, r) for d in range(pairs) for r in (1, 0)]
    peers = [spot for spot in spots if far(*spot)]

    barrier = pltpu.get_barrier_semaphore()
    for k in range(1, nz * nx):
        pl.semaphore_signal(
            barrier, inc=1, device_id={"ep": (me + k) % (nz * nx)}, device_id_type=MESH
        )
    pl.semaphore_signal(barrier, inc=1, device_id={"tp": other}, device_id_type=MESH)
    own.wait()
    pl.semaphore_wait(barrier, nz * nx)

    def remote(src, dst, send, recv, where):
        return pltpu.make_async_remote_copy(
            src_ref=src, dst_ref=dst, send_sem=send, recv_sem=recv,
            device_id=where, device_id_type=MESH,
        )

    def along(row):
        return {"ep": row * nx + x}

    across = {"ep": z * nx + beside}
    twin = {"tp": other}
    started = []

    def send(*what):
        copy = remote(*what)
        copy.start()
        started.append(copy)
        return copy

    block = xs.at[c, mine]
    send(block, block, fs.at[z], gr.at[mine], across)
    for d, r in peers:
        row = row_of(d, r)
        send(block, block, gs.at[row], gr.at[mine], along(row))
    send(block, block, ps.at[mine], pr.at[mine], twin)
    def arrive(j, d, r):
        if j == 0 and not far(d, r):
            return
        row = row_of(d, r)
        slot = (x + j) % nx * nz + row
        ref = xs.at[c, slot]
        remote(ref, ref, ps.at[slot], gr.at[slot], twin).wait_recv()
        if j == 0:
            send(ref, ref, fs.at[row], gr.at[slot], across)
        send(ref, ref, ps.at[slot], pr.at[slot], twin)

    theirs = pl.ds(pl.multiple_of(other * half, half), half)
    ours = pl.ds(pl.multiple_of(c * half, half), half)
    kept = {}

    def compute(j, d):
        for r in range(2):
            slot = (x + j) % nx * nz + row_of(d, r)
            ref = xs.at[other, slot]
            remote(ref, ref, ps.at[slot], pr.at[slot], twin).wait_recv()
        if (j, d) == (0, 0):
            weights[0].wait()
            weights[1].wait()
        base = (x + j) % nx * nz + 2 * ((z // 2 + d) % pairs)
        low = xs[0, pl.ds(base, 2)].reshape(2 * tok, half)
        high = xs[1, pl.ds(base, 2)].reshape(2 * tok, half)
        tile = min(256, hid)
        for at in range(0, hid, tile):
            cut = slice(at, at + tile)
            gate = jnp.dot(low, gw[:half, cut], preferred_element_type=jnp.float32)
            gate += jnp.dot(high, gw[half:, cut], preferred_element_type=jnp.float32)
            up = jnp.dot(low, uw[:half, cut], preferred_element_type=jnp.float32)
            up += jnp.dot(high, uw[half:, cut], preferred_element_type=jnp.float32)
            act[:, cut] = (jax.nn.silu(gate) * up).astype(jnp.bfloat16)
        if (j, d) == (0, 0):
            weights[2].wait()
        q = 2 * d + j
        psend[q] = jnp.dot(
            act[...], dw[:, theirs], preferred_element_type=jnp.float32
        ).astype(jnp.bfloat16)
        swap = remote(psend.at[q], precv.at[q], ds.at[q], dr.at[q], twin)
        swap.start()
        kept[q] = swap
        part = jnp.dot(act[...], dw[:, ours], preferred_element_type=jnp.float32)
        part = part.astype(jnp.bfloat16).reshape(2, tok, half)
        ys[pl.ds(base, 2)] = part

    eye = lax.broadcasted_iota(jnp.int32, (tok, tok), 0) == lax.broadcasted_iota(
        jnp.int32, (tok, tok), 1
    )

    def weight_of(chip):
        line = jnp.zeros((1, tok), jnp.float32)
        for k in range(ids.shape[0]):
            line += jnp.where(ids[k : k + 1] == chip, rw[k : k + 1], 0.0)
        return jnp.sum(jnp.where(eye, line, 0.0), axis=1, keepdims=True)

    def give_back(j, d):
        q = 2 * d + j
        kept[q].wait()
        column = (x + j) % nx
        for r in (1, 0):
            row = row_of(d, r)
            slot = column * nz + row
            got = precv[q, pl.ds(pl.multiple_of(row % 2 * tok, tok), tok)]
            done = ys[slot].astype(jnp.float32) + got.astype(jnp.float32)
            ys[slot] = done.astype(jnp.bfloat16)
            if j or far(d, r):
                send(
                    ys.at[slot], ret.at[mine], rs.at[slot], rr.at[mine],
                    {"ep": row * nx + column},
                )

    arrive(0, 0, 1)
    arrive(1, 0, 0)
    compute(0, 0)
    for d in range(1, pairs):
        arrive(0, d, 1)
        arrive(0, d, 0)
    arrive(1, 0, 1)
    give_back(0, 0)
    for d in range(1, pairs):
        compute(0, d)
    compute(1, 0)
    for d in range(1, pairs):
        give_back(0, d)
    for d in range(1, pairs):
        arrive(1, d, 1)
        arrive(1, d, 0)
    give_back(1, 0)
    for d in range(1, pairs):
        compute(1, d)
        give_back(1, d)

    own_ids.wait()
    own_rw.wait()
    total = weight_of(me) * ys[mine].astype(jnp.float32)
    for j, d, r in [(0, d, r) for d, r in peers] + [(1, d, r) for d, r in spots]:
        column, row = (x + j) % nx, row_of(d, r)
        slot = column * nz + row
        weight = weight_of(row * nx + column)
        remote(ret.at[slot], ret.at[slot], rs.at[slot], rr.at[slot], twin).wait_recv()
        total += weight * ret[slot].astype(jnp.float32)
    squares = jnp.sum(total * total, axis=1, keepdims=True)
    sq[...] = jnp.broadcast_to(squares, sq.shape)
    share = remote(sq, sqr, qs, qr, twin)
    share.start()
    own_gain.wait()
    share.wait()
    mean = (squares + sqr[:, :1]) / (half * 2)
    out[...] = (total * lax.rsqrt(mean + norm_eps) * gain[...]).astype(jnp.bfloat16)
    for copy in started:
        copy.wait_send()


def shards(hidden_state, expert_ids, route_weight, gate_matrix, up_matrix, down_matrix, norm_gain):
    tok, top = expert_ids.shape
    half = hidden_state.shape[1]
    hid = gate_matrix.shape[2]
    n = lax.axis_size("ep")
    if 2 * tok * top // n < tok or lax.axis_size("tp") != 2 or n % 4:
        return slotted(
            hidden_state, expert_ids, route_weight, gate_matrix, up_matrix, down_matrix, norm_gain
        )
    nx = 2
    nz = n // nx
    bf16, f32 = jnp.bfloat16, jnp.float32
    vmem = pl.BlockSpec(memory_space=pltpu.VMEM)
    dma = pltpu.SemaphoreType.DMA
    return pl.pallas_call(
        functools.partial(kernel, nz, nx),
        out_shape=jax.ShapeDtypeStruct((tok, half), bf16),
        in_specs=[pl.BlockSpec(memory_space=pl.ANY)] * 7,
        out_specs=vmem,
        scratch_shapes=[
            pltpu.VMEM((top, tok), jnp.int32),
            pltpu.VMEM((top, tok), f32),
            pltpu.VMEM((1, half), f32),
            pltpu.VMEM((2, n, tok, half), bf16),
            pltpu.VMEM((2 * half, hid), bf16),
            pltpu.VMEM((2 * half, hid), bf16),
            pltpu.VMEM((hid, 2 * half), bf16),
            pltpu.VMEM((2 * tok, hid), bf16),
            pltpu.VMEM((nz, 2 * tok, half), bf16),
            pltpu.VMEM((nz, 2 * tok, half), bf16),
            pltpu.VMEM((n, tok, half), bf16),
            pltpu.VMEM((n, tok, half), bf16),
            pltpu.VMEM((tok, 128), f32),
            pltpu.VMEM((tok, 128), f32),
            dma((3,)),
            dma((4,)),
            dma((nz,)),
            dma((n,)),
            dma((nz,)),
            dma((n,)),
            dma((n,)),
            dma((nz,)),
            dma((nz,)),
            dma((n,)),
            dma((n,)),
            dma,
            dma,
        ],
        compiler_params=pltpu.CompilerParams(
            collective_id=0, has_side_effects=True, vmem_limit_bytes=60 * 1024 * 1024
        ),
    )(
        expert_ids.T, route_weight.T, hidden_state, gate_matrix, up_matrix, down_matrix,
        norm_gain.reshape(1, half),
    )


def solution(mesh):
    placed = (
        P(("grp", "ep"), "tp"),
        P(("grp", "ep"), None),
        P(("grp", "ep"), None),
        P("ep", None, "tp"),
        P("ep", None, "tp"),
        P("ep", "tp", None),
        P("tp"),
    )
    return jax.shard_map(
        shards, mesh=mesh, in_specs=placed, out_specs=P(("grp", "ep"), "tp"), check_vma=False
    )
```

```python
import functools

import jax
import jax.numpy as jnp
from jax import lax
from jax.experimental import pallas as pl
from jax.experimental.pallas import tpu as pltpu
from jax.sharding import PartitionSpec as P

MESH = pl.DeviceIdType.MESH
norm_eps = 1e-05


def slot_numbers(block_ids, expert_count):
    onehot = (block_ids[..., None] == jnp.arange(expert_count, dtype=jnp.int32)).astype(jnp.int32)
    earlier = jnp.cumsum(onehot, axis=-2) - onehot
    return jnp.sum(earlier * onehot, axis=-1)


def expert_rows(buffer, gate_matrix, up_matrix, down_matrix):
    sources, item_count, feature_count = buffer.shape
    token_rows = buffer.reshape(sources * item_count, feature_count)
    gate_pre = jnp.dot(token_rows, gate_matrix[0], preferred_element_type=jnp.float32)
    up_pre = jnp.dot(token_rows, up_matrix[0], preferred_element_type=jnp.float32)
    activated = (jax.nn.silu(gate_pre) * up_pre).astype(jnp.bfloat16)
    partial_value = jnp.dot(activated, down_matrix[0], preferred_element_type=jnp.float32)
    return lax.psum_scatter(
        partial_value.reshape(sources, item_count, feature_count).astype(jnp.bfloat16),
        "tp",
        scatter_dimension=2,
        tiled=True,
    )


def slotted(hidden_state, expert_ids, route_weight, gate_matrix, up_matrix, down_matrix, norm_gain):
    tok_count, top_count = expert_ids.shape
    expert_count = lax.axis_size("ep")
    feature_total = hidden_state.shape[1] * lax.axis_size("tp")
    capacity = max(2, 2 * tok_count * top_count // expert_count)
    slot_total = expert_count * capacity
    slot_rank = slot_numbers(expert_ids.reshape(1, tok_count * top_count), expert_count)
    slot_index = expert_ids * capacity + slot_rank.reshape(tok_count, top_count)
    positions = jnp.arange(slot_total, dtype=jnp.int32)
    matches = slot_index[:, :, None] == positions[None, None, :]
    placing = jnp.transpose(jnp.any(matches, axis=1)).astype(jnp.bfloat16)
    combine = jnp.sum(jnp.where(matches, route_weight[:, :, None], 0.0), axis=1)
    outgoing = jnp.dot(placing, hidden_state, preferred_element_type=jnp.float32).astype(
        jnp.bfloat16
    )
    received = lax.all_to_all(
        outgoing.reshape(expert_count, capacity, hidden_state.shape[1]),
        "ep",
        split_axis=0,
        concat_axis=0,
        tiled=True,
    )
    answers = expert_rows(
        lax.all_gather(received, "tp", axis=2, tiled=True), gate_matrix, up_matrix, down_matrix
    )
    returned = lax.all_to_all(answers, "ep", split_axis=0, concat_axis=0, tiled=True)
    combined = jnp.dot(
        combine,
        returned.reshape(slot_total, returned.shape[2]).astype(jnp.float32),
        precision=lax.Precision.HIGHEST,
    )
    total_squares = lax.psum(jnp.sum(combined * combined, axis=1), "tp")
    inverse_rms = lax.rsqrt(total_squares / feature_total + norm_eps)
    return (combined * inverse_rms[:, None] * norm_gain).astype(jnp.bfloat16)


def kernel(
    nz, nx, ids_hbm, rw_hbm, h_hbm, g_hbm, u_hbm, d_hbm, gain_hbm, out,
    ids, rw, gain, xs, gw, uw, dw, act, psend, precv, ys, ret, sq, sqr,
    wsem, osem, gs, gr, fs, ps, pr, ds, dr, rs, rr, qs, qr,
):
    tok, half = out.shape
    hid = gw.shape[1]
    pairs = nz // 2
    me = lax.axis_index("ep")
    z, x = me // nx, me % nx
    beside = (x + 1) % nx
    c = lax.axis_index("tp")
    other = (c + 1) % 2
    mine = x * nz + z

    def local(src, dst, sem):
        copy = pltpu.make_async_copy(src, dst, sem)
        copy.start()
        return copy

    own = local(h_hbm, xs.at[c, mine], osem.at[0])
    own_ids = local(ids_hbm, ids, osem.at[1])
    own_rw = local(rw_hbm, rw, osem.at[2])
    weights = [
        local(g_hbm.at[0], gw, wsem.at[0]),
        local(u_hbm.at[0], uw, wsem.at[1]),
        local(d_hbm.at[0], dw, wsem.at[2]),
    ]
    own_gain = local(gain_hbm, gain, osem.at[3])

    def row_of(d, r):
        return 2 * ((z // 2 + d) % pairs) + (z + r) % 2

    def far(d, r):
        return (d, r) != (0, 0)

    spots = [(d, r) for d in range(pairs) for r in (1, 0)]
    peers = [spot for spot in spots if far(*spot)]

    barrier = pltpu.get_barrier_semaphore()
    for k in range(1, nz * nx):
        pl.semaphore_signal(
            barrier, inc=1, device_id={"ep": (me + k) % (nz * nx)}, device_id_type=MESH
        )
    pl.semaphore_signal(barrier, inc=1, device_id={"tp": other}, device_id_type=MESH)
    own.wait()
    pl.semaphore_wait(barrier, nz * nx)

    def remote(src, dst, send, recv, where):
        return pltpu.make_async_remote_copy(
            src_ref=src, dst_ref=dst, send_sem=send, recv_sem=recv,
            device_id=where, device_id_type=MESH,
        )

    def along(row):
        return {"ep": row * nx + x}

    across = {"ep": z * nx + beside}
    twin = {"tp": other}
    started = []

    def send(*what):
        copy = remote(*what)
        copy.start()
        started.append(copy)
        return copy

    block = xs.at[c, mine]
    send(block, block, fs.at[z], gr.at[mine], across)
    for d, r in peers:
        row = row_of(d, r)
        send(block, block, gs.at[row], gr.at[mine], along(row))
    send(block, block, ps.at[mine], pr.at[mine], twin)
    def arrive(j, d, r):
        if j == 0 and not far(d, r):
            return
        row = row_of(d, r)
        slot = (x + j) % nx * nz + row
        ref = xs.at[c, slot]
        remote(ref, ref, ps.at[slot], gr.at[slot], twin).wait_recv()
        if j == 0:
            send(ref, ref, fs.at[row], gr.at[slot], across)
        send(ref, ref, ps.at[slot], pr.at[slot], twin)

    theirs = pl.ds(pl.multiple_of(other * half, half), half)
    ours = pl.ds(pl.multiple_of(c * half, half), half)
    kept = {}

    def compute(j, d):
        for r in range(2):
            slot = (x + j) % nx * nz + row_of(d, r)
            ref = xs.at[other, slot]
            remote(ref, ref, ps.at[slot], pr.at[slot], twin).wait_recv()
        if (j, d) == (0, 0):
            weights[0].wait()
            weights[1].wait()
        base = (x + j) % nx * nz + 2 * ((z // 2 + d) % pairs)
        low = xs[0, pl.ds(base, 2)].reshape(2 * tok, half)
        high = xs[1, pl.ds(base, 2)].reshape(2 * tok, half)
        tile = min(256, hid)
        for at in range(0, hid, tile):
            cut = slice(at, at + tile)
            gate = jnp.dot(low, gw[:half, cut], preferred_element_type=jnp.float32)
            gate += jnp.dot(high, gw[half:, cut], preferred_element_type=jnp.float32)
            up = jnp.dot(low, uw[:half, cut], preferred_element_type=jnp.float32)
            up += jnp.dot(high, uw[half:, cut], preferred_element_type=jnp.float32)
            act[:, cut] = (jax.nn.silu(gate) * up).astype(jnp.bfloat16)
        if (j, d) == (0, 0):
            weights[2].wait()
        q = 2 * d + j
        psend[q] = jnp.dot(
            act[...], dw[:, theirs], preferred_element_type=jnp.float32
        ).astype(jnp.bfloat16)
        swap = remote(psend.at[q], precv.at[q], ds.at[q], dr.at[q], twin)
        swap.start()
        kept[q] = swap
        part = jnp.dot(act[...], dw[:, ours], preferred_element_type=jnp.float32)
        part = part.astype(jnp.bfloat16).reshape(2, tok, half)
        ys[pl.ds(base, 2)] = part

    eye = lax.broadcasted_iota(jnp.int32, (tok, tok), 0) == lax.broadcasted_iota(
        jnp.int32, (tok, tok), 1
    )

    def weight_of(chip):
        line = jnp.zeros((1, tok), jnp.float32)
        for k in range(ids.shape[0]):
            line += jnp.where(ids[k : k + 1] == chip, rw[k : k + 1], 0.0)
        return jnp.sum(jnp.where(eye, line, 0.0), axis=1, keepdims=True)

    def give_back(j, d):
        q = 2 * d + j
        kept[q].wait()
        column = (x + j) % nx
        for r in (1, 0):
            row = row_of(d, r)
            slot = column * nz + row
            got = precv[q, pl.ds(pl.multiple_of(row % 2 * tok, tok), tok)]
            done = ys[slot].astype(jnp.float32) + got.astype(jnp.float32)
            ys[slot] = done.astype(jnp.bfloat16)
            if j or far(d, r):
                send(
                    ys.at[slot], ret.at[mine], rs.at[slot], rr.at[mine],
                    {"ep": row * nx + column},
                )

    arrive(0, 0, 1)
    arrive(1, 0, 0)
    compute(0, 0)
    for d in range(1, pairs):
        arrive(0, d, 1)
        arrive(0, d, 0)
    arrive(1, 0, 1)
    give_back(0, 0)
    for d in range(1, pairs):
        compute(0, d)
    for d in range(1, pairs):
        give_back(0, d)
    compute(1, 0)
    give_back(1, 0)
    for d in range(1, pairs):
        arrive(1, d, 1)
        arrive(1, d, 0)
    for d in range(1, pairs):
        compute(1, d)
        give_back(1, d)

    own_ids.wait()
    own_rw.wait()
    total = weight_of(me) * ys[mine].astype(jnp.float32)
    for j, d, r in [(0, d, r) for d, r in peers] + [(1, d, r) for d, r in spots]:
        column, row = (x + j) % nx, row_of(d, r)
        slot = column * nz + row
        weight = weight_of(row * nx + column)
        remote(ret.at[slot], ret.at[slot], rs.at[slot], rr.at[slot], twin).wait_recv()
        total += weight * ret[slot].astype(jnp.float32)
    squares = jnp.sum(total * total, axis=1, keepdims=True)
    sq[...] = jnp.broadcast_to(squares, sq.shape)
    share = remote(sq, sqr, qs, qr, twin)
    share.start()
    own_gain.wait()
    share.wait()
    mean = (squares + sqr[:, :1]) / (half * 2)
    out[...] = (total * lax.rsqrt(mean + norm_eps) * gain[...]).astype(jnp.bfloat16)
    for copy in started:
        copy.wait_send()


def shards(hidden_state, expert_ids, route_weight, gate_matrix, up_matrix, down_matrix, norm_gain):
    tok, top = expert_ids.shape
    half = hidden_state.shape[1]
    hid = gate_matrix.shape[2]
    n = lax.axis_size("ep")
    if 2 * tok * top // n < tok or lax.axis_size("tp") != 2 or n % 4:
        return slotted(
            hidden_state, expert_ids, route_weight, gate_matrix, up_matrix, down_matrix, norm_gain
        )
    nx = 2
    nz = n // nx
    bf16, f32 = jnp.bfloat16, jnp.float32
    vmem = pl.BlockSpec(memory_space=pltpu.VMEM)
    dma = pltpu.SemaphoreType.DMA
    return pl.pallas_call(
        functools.partial(kernel, nz, nx),
        out_shape=jax.ShapeDtypeStruct((tok, half), bf16),
        in_specs=[pl.BlockSpec(memory_space=pl.ANY)] * 7,
        out_specs=vmem,
        scratch_shapes=[
            pltpu.VMEM((top, tok), jnp.int32),
            pltpu.VMEM((top, tok), f32),
            pltpu.VMEM((1, half), f32),
            pltpu.VMEM((2, n, tok, half), bf16),
            pltpu.VMEM((2 * half, hid), bf16),
            pltpu.VMEM((2 * half, hid), bf16),
            pltpu.VMEM((hid, 2 * half), bf16),
            pltpu.VMEM((2 * tok, hid), bf16),
            pltpu.VMEM((nz, 2 * tok, half), bf16),
            pltpu.VMEM((nz, 2 * tok, half), bf16),
            pltpu.VMEM((n, tok, half), bf16),
            pltpu.VMEM((n, tok, half), bf16),
            pltpu.VMEM((tok, 128), f32),
            pltpu.VMEM((tok, 128), f32),
            dma((3,)),
            dma((4,)),
            dma((nz,)),
            dma((n,)),
            dma((nz,)),
            dma((n,)),
            dma((n,)),
            dma((nz,)),
            dma((nz,)),
            dma((n,)),
            dma((n,)),
            dma,
            dma,
        ],
        compiler_params=pltpu.CompilerParams(
            collective_id=0, has_side_effects=True, vmem_limit_bytes=60 * 1024 * 1024
        ),
    )(
        expert_ids.T, route_weight.T, hidden_state, gate_matrix, up_matrix, down_matrix,
        norm_gain.reshape(1, half),
    )


def solution(mesh):
    placed = (
        P(("grp", "ep"), "tp"),
        P(("grp", "ep"), None),
        P(("grp", "ep"), None),
        P("ep", None, "tp"),
        P("ep", None, "tp"),
        P("ep", "tp", None),
        P("tp"),
    )
    return jax.shard_map(
        shards, mesh=mesh, in_specs=placed, out_specs=P(("grp", "ep"), "tp"), check_vma=False
    )
```
